256 devices in a mesh: ep: 16 (over y, x), tp: 16 (over z, core).
Axes of the slice: x: 4, y: 4, z: 8, core: 2. Of those that a mesh axis runs over, the one named last changes fastest.
Arguments:
- queries: bfloat16 [16384, 1024], P('ep', 'tp'), may hold values from -8 to 8
- keys: bfloat16 [16384, 256], P('ep'), may hold values from -8 to 8
- values: bfloat16 [16384, 256], P('ep'), may hold values from -6 to 6
- query_gain: float32 [64], replicated, may hold values from 1 to 10
- key_gain: float32 [64], replicated, may hold values from 1 to 10
- moe_input: bfloat16 [12288, 2048], P(('ep', 'tp')), may hold values from -6 to 6
- expert_ids: int32 [12288, 2], P('ep'), may hold values from 0 to 15, all different within a row; in each aligned block of 48 rows (0 to 47, 48 to 95, ...) at most 7 rows name the same one
- route_weight: float32 [12288, 2], P('ep'), may hold values from 0.2 to 1
- gate_weight: bfloat16 [16, 2048, 7168], P('ep', None, 'tp'), may hold values from -0.125 to 0.125
- up_weight: bfloat16 [16, 2048, 7168], P('ep', None, 'tp'), may hold values from -0.125 to 0.125
- down_weight: bfloat16 [16, 7168, 2048], P('ep', 'tp'), may hold values from -0.0625 to 0.0625
- output_gain: float32 [2048], replicated, may hold values from 0.1 to 1.9
Outputs:
- attended: bfloat16 [16384, 1024], P('ep', 'tp')
- moe_output: bfloat16 [12288, 2048], P(('ep', 'tp'))
The draws below stay inside these ranges and needn't reach their ends.
Inputs may be any that keep to these rules, and one draw needn't show every extreme that they name: `expert_ids`: the 2 experts of a token differ. In the rows of one device (aligned blocks of 48 tokens) no expert is named by more than 7 tokens, and in every draw some expert is named by exactly 7 tokens of some device.
All inputs are finite; a program needn't handle non-finite values.
Results may differ from the reference program's by a relative error of at most 0.0085.
The reference program's roundings to bfloat16 on the way count: a program that leaves them out, or rounds other values in their place, can miss the bound.
Values may be sent and summed in bfloat16 or wider, within the bound.
No kernel may reach another device: no remote copies, remote signals or barrier semaphores. Data moves between devices by JAX's collectives and lax.ppermute only.
A program may use at most 128 MiB of HBM per device.

```python
import math
import jax
import jax.numpy as jnp
import numpy as np
from jax import lax

D = 2048
HD = 64
QH = 16
KV = 4
GRID_W = 64
H_E = 7168
TOPK = 2
TOK_DEV = 48
LEN = 16384
TOKENS_B = 12288
EXPERTS = 16
CAP = 7
N_EP = 16
N_TP = 16


def draw_keys(key, part):
    normals = jax.random.normal(jax.random.fold_in(key, 31), (LEN, KV * HD), jnp.float32)
    return jnp.clip(normals, -8.0, 8.0).astype(jnp.bfloat16)


def draw_queries(key, part):
    normals = jax.random.normal(jax.random.fold_in(key, 33), (LEN, QH * HD), jnp.float32)
    return jnp.clip(normals, -8.0, 8.0).astype(jnp.bfloat16)


def draw_query_gain(key, part):
    seed_key = jax.random.fold_in(key, 41)
    return jnp.exp(jax.random.uniform(seed_key, (HD,), jnp.float32, 0.0, math.log(2.2)))


def draw_key_gain(key, part):
    seed_key = jax.random.fold_in(key, 43)
    return jnp.exp(jax.random.uniform(seed_key, (HD,), jnp.float32, 0.0, math.log(2.2)))


def block_levels(rng, shape, shards, low, largest):
    loudness = 1.0
    for dim, parts in shards:
        steps = jax.random.uniform(jax.random.fold_in(jax.random.fold_in(rng, 6), dim), (parts,), jnp.float32, low / len(shards), largest / len(shards))
        loudness = loudness * jnp.repeat(jnp.exp(steps), shape[dim] // parts).reshape((-1,) + (1,) * (len(shape) - 1 - dim))
    return loudness


def assign_block(key, own, number, rows, count, top, limit, slope):
    sequence = jax.random.permutation(key, count)
    heavy_load, usual = portions_of(count, rows * top, limit, slope, True), portions_of(count, rows * top, limit, slope, False)
    places = jnp.arange(count)

    def named(tallies, turn):
        used = int((tallies > 0).sum())
        fixed = max(1, used // 4)
        moved = fixed + (places - fixed + turn * (used - fixed)) % max(1, count - fixed)
        return jnp.zeros((count,), jnp.int32).at[sequence[jnp.where(places < fixed, places, moved)]].set(jnp.asarray(tallies, jnp.int32))

    tallies = jnp.where(number % 4 == 0, named(heavy_load, number // 4), named(usual, number - number // 4 - 1))
    mixed = jax.random.permutation(jax.random.fold_in(own, 3), count)
    source_of, sink = mixed[0:count // 2 * 2:2], mixed[1:count // 2 * 2:2]
    room = jnp.minimum(tallies[source_of] - 1, limit - tallies[sink]) // 2
    room = jnp.where((source_of == sequence[0]) | (sink == sequence[0]) | (tallies[sink] == 0), 0, jnp.maximum(room, 0))
    moved = jax.random.randint(jax.random.fold_in(own, 4), (count // 2,), 0, 1 << 20) % (room + 1)
    tallies = tallies.at[source_of].add(-moved).at[sink].add(moved)
    labels = jnp.searchsorted(jnp.cumsum(tallies), jnp.arange(rows * top), side="right").astype(jnp.int32)
    table = labels.reshape(top, rows).T
    table = table[jax.random.permutation(jax.random.fold_in(own, 1), rows)]
    turn = jax.random.randint(jax.random.fold_in(own, 2), (rows, 1), 0, top)
    return jnp.take_along_axis(table, (jnp.arange(top)[None, :] + turn) % top, axis=1)


def portions_of(number_of, total, limit, skew, full):
    portions = [(1 << 20) // math.isqrt(grade ** skew) + 1 for grade in range(1, number_of + 1)]
    largest = limit if full else min(limit, max(-(-total // number_of), total * portions[0] // sum(portions)))
    least = 1 if total - largest >= number_of - 1 else 0
    counts, spare = [largest] + [least] * (number_of - 1), total - largest - least * (number_of - 1)
    while spare > 0:
        movable = [i for i in range(1, number_of) if counts[i] < largest] or [i for i in range(1, number_of) if counts[i] < limit]
        mass, remaining = sum([portions[i] for i in movable]), spare
        for i in movable:
            addition = min(limit - counts[i], max(1, remaining * portions[i] // mass), spare)
            counts[i] = counts[i] + addition
            spare = spare - addition
    return np.array(counts)


def centred(own_key, dims, scale, reach, shards=(), held_as=jnp.bfloat16):
    level = block_levels(own_key, dims, shards, -0.22, 0.18) if shards else 1.0
    drawn = jax.random.normal(own_key, dims, jnp.float32) * scale * level
    return jnp.minimum(jnp.maximum(drawn, -reach), reach).astype(held_as)


def setup_inputs(seed: int = 0) -> dict:
    seeds = jax.random.split(jax.random.key(seed), 13)
    queries = draw_queries(jax.random.fold_in(seeds[12], 71), 0)
    keys = draw_keys(jax.random.fold_in(seeds[12], 71), 0)
    values = centred(seeds[2], (LEN, KV * HD), 1.0, 6.0, ((0, 16),))
    query_gain = draw_query_gain(jax.random.fold_in(seeds[12], 71), 0)
    key_gain = draw_key_gain(jax.random.fold_in(seeds[12], 71), 0)
    moe_input = centred(seeds[5], (TOKENS_B, D), 1.0, 6.0, ((0, 256),))
    expert_ids_keys = jax.random.split(jax.random.fold_in(seeds[6], 1), TOKENS_B // TOK_DEV)
    expert_ids_turns = jax.random.permutation(jax.random.fold_in(seeds[6], 3), TOKENS_B // TOK_DEV)
    expert_ids = jax.vmap(lambda own, number: assign_block(jax.random.fold_in(seeds[6], 2), own, number, TOK_DEV, EXPERTS, TOPK, CAP, 1))(expert_ids_keys, expert_ids_turns).reshape((TOKENS_B, TOPK))
    route_weight = jnp.clip(0.2 + 0.8 * jax.random.uniform(seeds[7], (TOKENS_B, TOPK), jnp.float32) ** block_levels(seeds[7], (TOKENS_B, TOPK), ((0, 16),), -0.2, 0.2), 0.2, 1.0)
    gate_weight = centred(seeds[8], (EXPERTS, D, H_E), D ** -0.5, 0.125, ((0, 16), (2, 16)))
    up_weight = centred(seeds[9], (EXPERTS, D, H_E), D ** -0.5, 0.125, ((0, 16), (2, 16)))
    down_weight = centred(seeds[10], (EXPERTS, H_E, D), H_E ** -0.5, 0.0625, ((0, 16), (1, 16)))
    output_gain = jnp.clip(1.0 + 0.18 * jax.random.normal(seeds[11], (D,), jnp.float32), 0.1, 1.9)
    return {"queries": queries, "keys": keys, "values": values, "query_gain": query_gain, "key_gain": key_gain, "moe_input": moe_input, "expert_ids": expert_ids, "route_weight": route_weight, "gate_weight": gate_weight, "up_weight": up_weight, "down_weight": down_weight, "output_gain": output_gain}


rope_theta = 10000.0
rms_epsilon = 1e-06
norm_epsilon = 1e-05
residual_scale = 1.4142135623730951

def unit_heads(heads, gain_vector):
    squares = lax.optimization_barrier(jnp.mean(heads * heads, axis=-1, keepdims=True))
    return heads * lax.rsqrt(squares + rms_epsilon) * gain_vector

def rotate_grid(heads, first_position, grid_width):
    head_size = heads.shape[-1]
    pair_count = head_size // 4
    position = first_position + jnp.arange(heads.shape[1], dtype=jnp.int32)
    grid_row = (position // grid_width).astype(jnp.float32)
    grid_col = (position % grid_width).astype(jnp.float32)
    inverse = rope_theta ** (-jnp.arange(pair_count, dtype=jnp.float32) / pair_count)
    angles = jnp.concatenate([grid_row[:, None] * inverse, grid_col[:, None] * inverse], axis=-1)
    cosines = jnp.cos(angles)
    sines = jnp.sin(angles)
    half_size = head_size // 2
    first_half = heads[..., :half_size]
    second_half = heads[..., half_size:]
    return jnp.concatenate([first_half * cosines - second_half * sines, second_half * cosines + first_half * sines], axis=-1)

def place_rank(choices, expert_count):
    matches = (choices[..., None] == jnp.arange(expert_count, dtype=jnp.int32)).astype(jnp.int32)
    earlier = jnp.cumsum(matches, axis=1) - matches
    return lax.optimization_barrier(jnp.sum(earlier * matches, axis=-1)).astype(jnp.int32)

def attention(queries, keys, values, query_gain, key_gain):
    length = queries.shape[0]
    query_heads = queries.reshape(length, QH, HD).transpose(1, 0, 2).astype(jnp.float32)
    rotated_queries = rotate_grid(unit_heads(query_heads, query_gain), 0, GRID_W).astype(jnp.bfloat16)
    key_heads = keys.reshape(length, KV, HD).transpose(1, 0, 2).astype(jnp.float32)
    rotated_keys = rotate_grid(unit_heads(key_heads, key_gain), 0, GRID_W).astype(jnp.bfloat16)
    value_heads = values.reshape(length, KV, HD).transpose(1, 0, 2)
    query_block = math.gcd(length, 1024)
    group_size = QH // KV
    score_scale = HD ** (-0.5)

    def one_head(head_index):
        key_rows = lax.dynamic_index_in_dim(rotated_keys, head_index // group_size, 0, keepdims=False)
        value_rows = lax.dynamic_index_in_dim(value_heads, head_index // group_size, 0, keepdims=False)
        query_rows = lax.dynamic_index_in_dim(rotated_queries, head_index, 0, keepdims=False)

        def one_block(query_part):
            scores = jnp.dot(query_part, key_rows.T, preferred_element_type=jnp.float32) * score_scale
            row_max = lax.optimization_barrier(jnp.max(scores, axis=-1, keepdims=True))
            weights = jnp.exp(scores - row_max)
            totals = lax.optimization_barrier(jnp.sum(weights, axis=-1, keepdims=True))
            summed = jnp.dot(weights.astype(jnp.bfloat16), value_rows, preferred_element_type=jnp.float32)
            return (summed / totals).astype(jnp.bfloat16)
        blocks = query_rows.reshape(length // query_block, query_block, HD)
        return lax.map(one_block, blocks).reshape(length, HD)
    attended = lax.map(one_head, jnp.arange(QH, dtype=jnp.int32))
    return attended.transpose(1, 0, 2).reshape(length, QH * HD)

def run_expert(operands):
    expert_rows, gate_matrix, up_matrix, down_matrix = operands
    gate_part = jnp.dot(expert_rows, gate_matrix, preferred_element_type=jnp.float32)
    up_part = jnp.dot(expert_rows, up_matrix, preferred_element_type=jnp.float32)
    hidden = (jax.nn.silu(gate_part) * up_part).astype(jnp.bfloat16)
    group_width = hidden.shape[1] // N_TP
    hidden_groups = hidden.reshape(hidden.shape[0], N_TP, group_width).transpose(1, 0, 2)
    down_groups = down_matrix.reshape(N_TP, group_width, down_matrix.shape[1])

    def add_group(running, operand_pair):
        hidden_part, down_part = operand_pair
        partial_sum = jnp.dot(hidden_part, down_part, preferred_element_type=jnp.float32)
        rounded = lax.optimization_barrier(partial_sum.astype(jnp.bfloat16))
        return (running + rounded.astype(jnp.float32), None)
    start_sum = jnp.zeros((hidden.shape[0], down_matrix.shape[1]), jnp.float32)
    summed, ignored = lax.scan(add_group, start_sum, (hidden_groups, down_groups))
    return summed.astype(jnp.bfloat16)

def layer_scale(mixed, gain_vector):
    average = lax.optimization_barrier(jnp.mean(mixed, axis=-1, keepdims=True))
    centered = mixed - average
    variance = lax.optimization_barrier(jnp.mean(centered * centered, axis=-1, keepdims=True))
    return (centered * lax.rsqrt(variance + norm_epsilon) * gain_vector).astype(jnp.bfloat16)

def experts_layer(moe_input, expert_ids, route_weight, gate_weight, up_weight, down_weight, output_gain):
    top_count = expert_ids.shape[1]
    block_count = N_EP * N_TP
    choices = expert_ids.reshape(block_count, TOK_DEV * top_count)
    ranks = place_rank(choices, EXPERTS)
    expert_span = block_count * CAP
    targets = choices * expert_span + jnp.arange(block_count, dtype=jnp.int32)[:, None] * CAP + ranks
    tokens_from = jnp.arange(block_count * TOK_DEV * top_count, dtype=jnp.int32) // top_count
    sources = jnp.full((EXPERTS * expert_span,), block_count * TOK_DEV, jnp.int32).at[targets.reshape(-1)].set(tokens_from)
    gathered = jnp.take(moe_input, sources, axis=0, mode='fill', fill_value=0).reshape(EXPERTS, expert_span, D)
    outputs = lax.map(run_expert, (gathered, gate_weight, up_weight, down_weight))
    picked = jnp.take(outputs.reshape(EXPERTS * expert_span, D), targets.reshape(-1), axis=0)
    picked = picked.reshape(block_count * TOK_DEV, top_count, D).astype(jnp.float32)
    mixed = residual_scale * moe_input.astype(jnp.float32) + lax.optimization_barrier(jnp.sum(route_weight[:, :, None] * picked, axis=1))
    return layer_scale(mixed, output_gain)

def reference(queries, keys, values, query_gain, key_gain, moe_input, expert_ids, route_weight, gate_weight, up_weight, down_weight, output_gain):
    attended = attention(queries, keys, values, query_gain, key_gain)
    moe_output = experts_layer(moe_input, expert_ids, route_weight, gate_weight, up_weight, down_weight, output_gain)
    return (attended, moe_output)
```

```python
import functools
import math

import jax
import jax.numpy as jnp
import numpy as np
from jax import lax
from jax.experimental import pallas as pl
from jax.experimental.pallas import tpu as pltpu
from jax.sharding import Mesh
from jax.sharding import PartitionSpec as P

KV = 4
GRID_W = 64
TP = ("tp_0", "tp_1")
EP_TP = ("ep", "tp_0", "tp_1")
CAP = 7
HD = 64
HALF = HD // 2
PAIRS = HD // 4
LOG2E = math.log2(math.e)

rope_theta = 10000.0
rms_epsilon = 1e-06
norm_epsilon = 1e-05
residual_scale = 1.4142135623730951

F32 = jnp.float32
BF16 = jnp.bfloat16
VMEM_LIMIT = 56 * 1024 * 1024


def dot(a, b, contract=((1,), (0,))):
    return lax.dot_general(a, b, (contract, ((), ())), preferred_element_type=F32)


def angle_tables(count):
    inverse = (np.float32(rope_theta) ** (-np.arange(PAIRS, dtype=np.float32) / np.float32(PAIRS))).astype(np.float32)
    angles = np.arange(count, dtype=np.float32)[:, None] * inverse
    return np.concatenate([np.cos(angles), np.sin(angles)], axis=1).astype(np.float32)


def spread(row_table, col_table):
    rows = row_table.shape[0]
    width = row_table.shape[1]
    by_row = jnp.broadcast_to(row_table[:, None, :], (rows, GRID_W, width)).reshape(rows * GRID_W, width)
    by_col = jnp.broadcast_to(col_table[None, :, :], (rows, GRID_W, width)).reshape(rows * GRID_W, width)
    cosines = jnp.concatenate([by_row[:, :PAIRS], by_col[:, :PAIRS]], axis=1)
    sines = jnp.concatenate([by_row[:, PAIRS:], by_col[:, PAIRS:]], axis=1)
    return cosines, sines


def rotate(heads, gain, cosines, sines):
    squares = jnp.mean(heads * heads, axis=-1, keepdims=True)
    heads = heads * lax.rsqrt(squares + rms_epsilon) * gain
    a = heads[:, :HALF]
    b = heads[:, HALF:]
    return jnp.concatenate([a * cosines - b * sines, b * cosines + a * sines], axis=1)


def key_kernel(place, keys, values, gain, row_table, col_table, out):
    low = place[1] == 0
    k = jnp.where(low, keys[:, :HD], keys[:, HD:]).astype(F32)
    v = jnp.where(low, values[:, :HD], values[:, HD:])
    cosines, sines = spread(row_table[...], col_table[...])
    out[...] = jnp.concatenate([rotate(k, gain[...], cosines, sines).astype(BF16), v], axis=1)


def query_kernel(place, queries, gain, row_table, col_table, out):
    cosines, sines = spread(row_table[...], col_table[...])
    q = rotate(queries[...].astype(F32), gain[...], cosines, sines).astype(BF16)
    scaled = q.astype(F32) * F32(LOG2E * HD**-0.5)
    high = scaled.astype(BF16)
    out[...] = jnp.concatenate([high, (scaled - high.astype(F32)).astype(BF16)], axis=1)


def attend_kernel(q_ref, near_ref, far_ref, out_ref, kk_ref, v1_ref, top_ref, acc_ref, *, block_q, steps):
    step = pl.program_id(0)
    block_k = kk_ref.shape[0]

    def stage(kv):
        lane = lax.broadcasted_iota(jnp.int32, kv.shape, 1)
        kk_ref[...] = jnp.concatenate([kv[:, :HD], kv[:, :HD]], axis=1)
        v1_ref[...] = jnp.where(lane < HD, jnp.ones_like(kv), kv)

    @pl.when(step < steps)
    def _():
        stage(near_ref[...])

    @pl.when(step >= steps)
    def _():
        stage(far_ref[...])

    count = q_ref.shape[0] // block_q

    @pl.when(step == 0)
    def _():
        for t in range(count):
            rows = pl.ds(t * block_q, block_q)
            s = dot(q_ref[rows, :], kk_ref[:256, :], ((1,), (1,)))
            top_ref[rows, :] = jnp.broadcast_to(jnp.max(s, axis=1, keepdims=True), (block_q, 128))
        acc_ref[...] = jnp.zeros_like(acc_ref)

    def weigh(q, top, k):
        s = dot(q, kk_ref[pl.ds(k * 256, 256), :], ((1,), (1,)))
        p = jnp.exp2(s - jnp.concatenate([top, top], axis=1)).astype(BF16)
        return dot(p, v1_ref[pl.ds(k * 256, 256), :])

    def tile(t, carry):
        rows = pl.ds(pl.multiple_of(t * block_q, block_q), block_q)
        q = q_ref[rows, :]
        top = top_ref[rows, :]
        part = jnp.zeros((block_q, 128), F32)
        for k in range(block_k // 256):
            part = part + weigh(q, top, k)
        over = jnp.max(jnp.where(part[:, :1] < 2.0**100, 0.0, 1.0)) > 0

        @pl.when(jnp.logical_not(over))
        def _():
            acc_ref[rows, :] += part

        @pl.when(over)
        def _():
            def raise_top(k, peak):
                s = dot(q, kk_ref[pl.ds(pl.multiple_of(k * 256, 256), 256), :], ((1,), (1,)))
                return jnp.maximum(peak, jnp.max(s, axis=1, keepdims=True))

            peak = lax.fori_loop(0, block_k // 256, raise_top, jnp.max(top, axis=1, keepdims=True))
            peak = jnp.broadcast_to(peak, (block_q, 128))
            acc_ref[rows, :] = acc_ref[rows, :] * jnp.exp2(top - peak)
            top_ref[rows, :] = peak

            def add(k, carry):
                acc_ref[rows, :] += weigh(q, peak, pl.multiple_of(k, 1))
                return carry

            lax.fori_loop(0, block_k // 256, add, 0)

        return carry

    lax.fori_loop(0, count, tile, 0)

    @pl.when(step == 2 * steps - 1)
    def _():
        a = acc_ref[...]
        out_ref[...] = (a[:, HD:] / a[:, :HD]).astype(BF16)


def attend(q, near, far, block_q=512, block_k=4096):
    rows = q.shape[0]
    steps = near.shape[0] // block_k
    return pl.pallas_call(
        functools.partial(attend_kernel, block_q=block_q, steps=steps),
        grid=(2 * steps,),
        in_specs=[
            pl.BlockSpec((rows, 128), lambda j: (0, 0)),
            pl.BlockSpec((block_k, 128), lambda j: (jnp.minimum(j, steps - 1), 0)),
            pl.BlockSpec((block_k, 128), lambda j: (jnp.maximum(j - steps, 0), 0)),
        ],
        out_specs=pl.BlockSpec((rows, HD), lambda j: (0, 0)),
        out_shape=jax.ShapeDtypeStruct((rows, HD), BF16),
        scratch_shapes=[
            pltpu.VMEM((block_k, 128), BF16),
            pltpu.VMEM((block_k, 128), BF16),
            pltpu.VMEM((rows, 128), F32),
            pltpu.VMEM((rows, 128), F32),
        ],
        compiler_params=pltpu.CompilerParams(vmem_limit_bytes=VMEM_LIMIT),
        cost_estimate=pl.CostEstimate(
            flops=rows * near.shape[0] * 2 * 256 * 4, transcendentals=0, bytes_accessed=near.size * 4
        ),
        name="attend",
    )(q, near, far)


def slots_of(ids, experts):
    tokens = ids.shape[0]
    width = experts * CAP
    slot = lax.broadcasted_iota(jnp.int32, (tokens, width), 1)
    owner = jnp.zeros((tokens, width), jnp.int32)
    for e in range(1, experts):
        owner = owner + (slot >= e * CAP).astype(jnp.int32)
    first = ids[:, 0:1] == owner
    second = ids[:, 1:2] == owner
    named = jnp.where(first | second, 1.0, 0.0)
    row = lax.broadcasted_iota(jnp.int32, (tokens, tokens), 0)
    col = lax.broadcasted_iota(jnp.int32, (tokens, tokens), 1)
    before = dot(jnp.where(col < row, 1.0, 0.0).astype(BF16), named.astype(BF16))
    rank = (slot - owner * CAP).astype(F32)
    taken = (named > 0) & (before == rank)
    return taken, first


def dispatch_kernel(place, ids, rows, out, *, experts):
    taken, ignored = slots_of(ids[...], experts)
    out[...] = dot(jnp.where(taken, 1.0, 0.0).astype(BF16), rows[...], ((0,), (0,))).astype(BF16)


def combine_kernel(place, ids, weights, rows, returned, gain, out, *, experts):
    taken, first = slots_of(ids[...], experts)
    w = weights[...]
    scale = jnp.where(taken, jnp.where(first, w[:, 0:1], w[:, 1:2]), 0.0)
    high = scale.astype(BF16)
    rest = scale - high.astype(F32)
    mid = rest.astype(BF16)
    low = (rest - mid.astype(F32)).astype(BF16)
    back = returned[...]
    mixed = residual_scale * rows[...].astype(F32) + (dot(high, back) + dot(mid, back) + dot(low, back))
    average = jnp.mean(mixed, axis=-1, keepdims=True)
    centered = mixed - average
    variance = jnp.mean(centered * centered, axis=-1, keepdims=True)
    out[...] = (centered * lax.rsqrt(variance + norm_epsilon) * gain[...]).astype(BF16)


def expert_kernel(x_ref, *refs):
    weights, out_ref, bufs, sems = refs[:6], refs[6], refs[7:13], refs[13]
    copies = [pltpu.make_async_copy(w, b, sems.at[i]) for i, (w, b) in enumerate(zip(weights, bufs))]
    for c in copies:
        c.start()
    x = x_ref[...]
    total = None
    for half in range(2):
        gate_b, up_b, down_b = bufs[3 * half : 3 * half + 3]
        copies[3 * half].wait()
        gate = dot(x, gate_b[...])
        copies[3 * half + 1].wait()
        up = dot(x, up_b[...])
        hidden = (gate / (1.0 + jnp.exp(-gate)) * up).astype(BF16)
        copies[3 * half + 2].wait()
        part = dot(hidden, down_b[...])
        total = part if total is None else total + part
    out_ref[...] = total.astype(BF16)


def run_expert(x, weights):
    rows, width = x.shape
    any_spec = pl.BlockSpec(memory_space=pl.ANY)
    return pl.pallas_call(
        expert_kernel,
        in_specs=[pl.BlockSpec((rows, width), lambda: (0, 0))] + [any_spec] * 6,
        out_specs=pl.BlockSpec((rows, width), lambda: (0, 0)),
        out_shape=jax.ShapeDtypeStruct((rows, width), BF16),
        scratch_shapes=[pltpu.VMEM(w.shape, BF16) for w in weights] + [pltpu.SemaphoreType.DMA((6,))],
        compiler_params=pltpu.CompilerParams(vmem_limit_bytes=VMEM_LIMIT),
        cost_estimate=pl.CostEstimate(
            flops=rows * sum(w.size for w in weights) * 2, transcendentals=0, bytes_accessed=2 * sum(w.size for w in weights)
        ),
        name="expert",
    )(x, *weights)


def place_call(body, place, specs, out_block, out_shape, name):
    return pl.pallas_call(
        body,
        grid_spec=pltpu.PrefetchScalarGridSpec(num_scalar_prefetch=1, grid=(1,), in_specs=specs, out_specs=out_block),
        out_shape=out_shape,
        compiler_params=pltpu.CompilerParams(vmem_limit_bytes=VMEM_LIMIT),
        name=name,
    )


def shards(
    queries,
    keys,
    values,
    query_gain,
    key_gain,
    moe_input,
    expert_ids,
    route_weight,
    gate_weight,
    up_weight,
    down_weight,
    output_gain,
):
    seg_rows = queries.shape[0]
    half_rows = seg_rows // 2
    tok_rows, model_width = moe_input.shape
    experts = lax.axis_size("ep")
    column = lax.axis_index(TP)
    ep = lax.axis_index("ep")
    core = lax.axis_index("tp_1")
    key_head = column * KV // lax.axis_size(TP)
    place = jnp.stack([key_head // 2, key_head % 2, ep, core, column]).astype(jnp.int32)

    whole = lambda shape: pl.BlockSpec(shape, lambda i, p: (0, 0))
    own = pl.BlockSpec((tok_rows, 2), lambda i, p: (p[4], 0))
    slots = experts * CAP
    outgoing = place_call(
        functools.partial(dispatch_kernel, experts=experts),
        place,
        [own, whole((tok_rows, model_width))],
        whole((slots, model_width)),
        jax.ShapeDtypeStruct((slots, model_width), BF16),
        "dispatch",
    )(place, expert_ids, moe_input)
    arrived = lax.all_to_all(
        outgoing.reshape(experts, CAP, model_width), "ep", split_axis=0, concat_axis=0, tiled=True
    ).reshape(slots, model_width)

    own_weights = (gate_weight[0], up_weight[0], down_weight[0])
    swap = [(0, 1), (1, 0)]
    other_weights = tuple(lax.ppermute(w, "tp_1", swap) for w in own_weights)

    row_table = jnp.asarray(angle_tables(seg_rows * experts // GRID_W))
    col_table = jnp.asarray(angle_tables(GRID_W))
    kv_grid = half_rows // GRID_W
    kv_rows = pl.BlockSpec((half_rows, 128), lambda i, p: (p[3], p[0]))
    kv_own = place_call(
        key_kernel,
        place,
        [
            kv_rows,
            kv_rows,
            whole((1, HD)),
            pl.BlockSpec((kv_grid, 2 * PAIRS), lambda i, p: (2 * p[2] + p[3], 0)),
            whole((GRID_W, 2 * PAIRS)),
        ],
        whole((half_rows, 2 * HD)),
        jax.ShapeDtypeStruct((half_rows, 2 * HD), BF16),
        "keys",
    )(place, keys, values, key_gain[None], row_table, col_table)
    kv_near = lax.all_gather(kv_own, "ep", axis=0, tiled=True)
    kv_far = lax.ppermute(kv_near, "tp_1", swap)
    q = place_call(
        query_kernel,
        place,
        [
            whole((seg_rows, HD)),
            whole((1, HD)),
            pl.BlockSpec((seg_rows // GRID_W, 2 * PAIRS), lambda i, p: (p[2], 0)),
            whole((GRID_W, 2 * PAIRS)),
        ],
        whole((seg_rows, 2 * HD)),
        jax.ShapeDtypeStruct((seg_rows, 2 * HD), BF16),
        "queries",
    )(place, queries, query_gain[None], row_table, col_table)

    gathered = lax.all_gather(arrived, "tp_0", axis=0, tiled=True)
    partial = run_expert(gathered, own_weights + other_weights)
    expert_out = lax.psum_scatter(partial, "tp_0", scatter_dimension=0, tiled=True)
    attended = attend(q, kv_near, kv_far)
    returned = lax.all_to_all(
        expert_out.reshape(experts, CAP, model_width), "ep", split_axis=0, concat_axis=0, tiled=True
    ).reshape(slots, model_width)
    moe_output = place_call(
        functools.partial(combine_kernel, experts=experts),
        place,
        [own, own, whole((tok_rows, model_width)), whole((slots, model_width)), whole((1, model_width))],
        whole((tok_rows, model_width)),
        jax.ShapeDtypeStruct((tok_rows, model_width), BF16),
        "combine",
    )(place, expert_ids, route_weight, moe_input, returned, output_gain[None])
    return (attended, moe_output)


def solution(mesh):
    split = Mesh(mesh.devices.reshape(mesh.shape["ep"], 8, 2), ("ep", "tp_0", "tp_1"))
    return jax.shard_map(
        shards,
        mesh=split,
        in_specs=(
            P("ep", TP),
            P("ep", None),
            P("ep", None),
            P(),
            P(),
            P(EP_TP, None),
            P("ep", None),
            P("ep", None),
            P("ep", None, TP),
            P("ep", None, TP),
            P("ep", TP, None),
            P(),
        ),
        out_specs=(P("ep", TP), P(EP_TP, None)),
        check_vma=False,
    )
```

```python
import functools
import math

import jax
import jax.numpy as jnp
import numpy as np
from jax import lax
from jax.experimental import pallas as pl
from jax.experimental.pallas import tpu as pltpu
from jax.sharding import Mesh
from jax.sharding import PartitionSpec as P


KV = 4
GRID_W = 64
TP = ("tp_0", "tp_1")
EP_TP = ("ep", "tp_0", "tp_1")
CAP = 7
HD = 64
HALF = HD // 2
PAIRS = HD // 4
LOG2E = math.log2(math.e)

rope_theta = 10000.0
rms_epsilon = 1e-06
norm_epsilon = 1e-05
residual_scale = 1.4142135623730951

F32 = jnp.float32
BF16 = jnp.bfloat16
VMEM_LIMIT = 56 * 1024 * 1024


def dot(a, b, contract=((1,), (0,))):
    return lax.dot_general(a, b, (contract, ((), ())), preferred_element_type=F32)


def angle_tables(count):
    inverse = (np.float32(rope_theta) ** (-np.arange(PAIRS, dtype=np.float32) / np.float32(PAIRS))).astype(np.float32)
    angles = np.arange(count, dtype=np.float32)[:, None] * inverse
    return np.concatenate([np.cos(angles), np.sin(angles)], axis=1).astype(np.float32)


def spread(row_table, col_table):
    rows = row_table.shape[0]
    width = row_table.shape[1]
    by_row = jnp.broadcast_to(row_table[:, None, :], (rows, GRID_W, width)).reshape(rows * GRID_W, width)
    by_col = jnp.broadcast_to(col_table[None, :, :], (rows, GRID_W, width)).reshape(rows * GRID_W, width)
    cosines = jnp.concatenate([by_row[:, :PAIRS], by_col[:, :PAIRS]], axis=1)
    sines = jnp.concatenate([by_row[:, PAIRS:], by_col[:, PAIRS:]], axis=1)
    return cosines, sines


def rotate(heads, gain, cosines, sines):
    squares = jnp.mean(heads * heads, axis=-1, keepdims=True)
    heads = heads * lax.rsqrt(squares + rms_epsilon) * gain
    a = heads[:, :HALF]
    b = heads[:, HALF:]
    return jnp.concatenate([a * cosines - b * sines, b * cosines + a * sines], axis=1)


def key_kernel(place, keys, values, gain, row_table, col_table, out):
    low = place[1] == 0
    k = jnp.where(low, keys[:, :HD], keys[:, HD:]).astype(F32)
    v = jnp.where(low, values[:, :HD], values[:, HD:])
    cosines, sines = spread(row_table[...], col_table[...])
    kv = jnp.concatenate([rotate(k, gain[...], cosines, sines).astype(BF16), v], axis=1)
    out[...] = jnp.broadcast_to(kv[None], out.shape)


def query_kernel(place, queries, gain, row_table, col_table, out):
    cosines, sines = spread(row_table[...], col_table[...])
    q = rotate(queries[...].astype(F32).T, gain[...], cosines, sines).astype(BF16)
    scaled = q.astype(F32) * F32(LOG2E * HD**-0.5)
    high = scaled.astype(BF16)
    out[...] = jnp.concatenate([high, (scaled - high.astype(F32)).astype(BF16)], axis=1)


def attend_kernel(*refs, block_q, first, last):
    q_ref, kv_ref = refs[:2]
    refs = refs[2:]
    if first:
        acc_in = top_in = None
    else:
        acc_in, top_in = refs[:2]
        refs = refs[2:]
    if last:
        out_ref, kk_ref, v1_ref, top_ref, acc_ref = refs
    else:
        acc_ref, top_ref, kk_ref, v1_ref = refs
    block_k = kk_ref.shape[0]
    count = q_ref.shape[0] // block_q
    kv = kv_ref[...]
    lane = lax.broadcasted_iota(jnp.int32, kv.shape, 1)
    kk_ref[...] = jnp.concatenate([kv[:, :HD], kv[:, :HD]], axis=1)
    v1_ref[...] = jnp.where(lane < HD, jnp.ones_like(kv), kv)

    @pl.when(pl.program_id(0) == 0)
    def _():
        if first:
            for t in range(count):
                rows = pl.ds(t * block_q, block_q)
                s = dot(q_ref[rows, :], kk_ref[:256, :], ((1,), (1,)))
                top_ref[rows, :] = jnp.broadcast_to(jnp.max(s, axis=1, keepdims=True), (block_q, 128))
            acc_ref[...] = jnp.zeros_like(acc_ref)
        else:
            top_ref[...] = top_in[...]
            acc_ref[...] = acc_in[...]

    def weigh(q, top, at):
        s = dot(q, kk_ref[pl.ds(at, 256), :], ((1,), (1,)))
        p = jnp.exp2(s - jnp.concatenate([top, top], axis=1)).astype(BF16)
        return dot(p, v1_ref[pl.ds(at, 256), :])

    def tile(t, carry):
        rows = pl.ds(pl.multiple_of(t * block_q, block_q), block_q)
        q = q_ref[rows, :]
        top = top_ref[rows, :]
        part = jnp.zeros((block_q, 128), F32)
        for k in range(block_k // 256):
            part = part + weigh(q, top, k * 256)
        over = jnp.max(jnp.where(part[:, :1] < 2.0**100, 0.0, 1.0)) > 0

        @pl.when(jnp.logical_not(over))
        def _():
            acc_ref[rows, :] += part

        @pl.when(over)
        def _():
            def raise_top(k, peak):
                s = dot(q, kk_ref[pl.ds(pl.multiple_of(k * 256, 256), 256), :], ((1,), (1,)))
                return jnp.maximum(peak, jnp.max(s, axis=1, keepdims=True))

            peak = lax.fori_loop(0, block_k // 256, raise_top, jnp.max(top, axis=1, keepdims=True))
            peak = jnp.broadcast_to(peak, (block_q, 128))
            acc_ref[rows, :] = acc_ref[rows, :] * jnp.exp2(top - peak)
            top_ref[rows, :] = peak

            def add(k, carry):
                acc_ref[rows, :] += weigh(q, peak, pl.multiple_of(k * 256, 256))
                return carry

            lax.fori_loop(0, block_k // 256, add, 0)

        return carry

    lax.fori_loop(0, count, tile, 0)

    if last:

        @pl.when(pl.program_id(0) == pl.num_programs(0) - 1)
        def _():
            a = acc_ref[...]
            out_ref[...] = (a[:, HD:] / a[:, :HD]).T.astype(BF16)


def attend(q, kv, start, keys, state=None, last=False, block_q=512, block_k=4096):
    rows = q.shape[0]
    steps = keys // block_k
    whole = pl.BlockSpec((rows, 128), lambda j: (0, 0))
    running = [jax.ShapeDtypeStruct((rows, 128), F32)] * 2
    scratch = [pltpu.VMEM((block_k, 128), BF16)] * 2
    if last:
        out_shape = jax.ShapeDtypeStruct((HD, rows), BF16)
        out_specs = pl.BlockSpec((HD, rows), lambda j: (0, 0))
        scratch = scratch + [pltpu.VMEM((rows, 128), F32)] * 2
    else:
        out_shape = running
        out_specs = [whole, whole]
    return pl.pallas_call(
        functools.partial(attend_kernel, block_q=block_q, first=state is None, last=last),
        grid=(steps,),
        in_specs=[whole, pl.BlockSpec((block_k, 128), lambda j: (j + start // block_k, 0))]
        + [whole] * (0 if state is None else 2),
        out_specs=out_specs,
        out_shape=out_shape,
        scratch_shapes=scratch,
        compiler_params=pltpu.CompilerParams(vmem_limit_bytes=VMEM_LIMIT),
        cost_estimate=pl.CostEstimate(flops=rows * keys * 2 * 256 * 2, transcendentals=0, bytes_accessed=keys * 256),
        name="attend",
    )(q, kv, *(() if state is None else state))


def own_tokens(place, table, tokens):
    width = table.shape[1]
    start = place[4] * tokens
    return pltpu.roll(table[...], jnp.where(start == 0, 0, width - start), 1)[:, :tokens]


def slots_of(ids, experts):
    tokens = ids.shape[1]
    width = experts * CAP
    slot = lax.broadcasted_iota(jnp.int32, (width, tokens), 0)
    owner = jnp.zeros((width, tokens), jnp.int32)
    for e in range(1, experts):
        owner = owner + (slot >= e * CAP).astype(jnp.int32)
    first = ids[0:1, :] == owner
    second = ids[1:2, :] == owner
    named = jnp.where(first | second, 1.0, 0.0)
    row = lax.broadcasted_iota(jnp.int32, (tokens, tokens), 0)
    col = lax.broadcasted_iota(jnp.int32, (tokens, tokens), 1)
    before = dot(named.astype(BF16), jnp.where(row < col, 1.0, 0.0).astype(BF16))
    rank = (slot - owner * CAP).astype(F32)
    taken = (named > 0) & (before == rank)
    return taken, first


def dispatch_kernel(place, ids, rows, out, *, experts):
    taken, _ = slots_of(own_tokens(place, ids, rows.shape[0]), experts)
    picked = dot(jnp.where(taken, 1.0, 0.0).astype(BF16), rows[...])
    for e in range(experts):
        out[e] = picked[e * CAP : (e + 1) * CAP].astype(BF16)


def combine_kernel(place, ids, weights, rows, returned, gain, out, *, experts):
    tokens = rows.shape[0]
    taken, first = slots_of(own_tokens(place, ids, tokens), experts)
    w = own_tokens(place, weights, tokens)
    scale = jnp.where(taken, jnp.where(first, w[0:1, :], w[1:2, :]), 0.0)
    high = scale.astype(BF16)
    rest = scale - high.astype(F32)
    mid = rest.astype(BF16)
    low = (rest - mid.astype(F32)).astype(BF16)
    back = returned[...]
    down = ((0,), (0,))
    mixed = residual_scale * rows[...].astype(F32) + (dot(high, back, down) + dot(mid, back, down) + dot(low, back, down))
    average = jnp.mean(mixed, axis=-1, keepdims=True)
    centered = mixed - average
    variance = jnp.mean(centered * centered, axis=-1, keepdims=True)
    out[...] = (centered * lax.rsqrt(variance + norm_epsilon) * gain[...]).astype(BF16)


def expert_kernel(*refs, blocks):
    xs, weights, outs = refs[:blocks], refs[blocks : blocks + 6], refs[blocks + 6 : -7]
    bufs, sems = refs[-7:-1], refs[-1]
    copies = [pltpu.make_async_copy(w, b, sems.at[i]) for i, (w, b) in enumerate(zip(weights, bufs))]
    for c in copies:
        c.start()
    x = xs[0][...] if blocks == 1 else jnp.concatenate([x[...] for x in xs], axis=0)
    total = None
    for half in range(2):
        gate_b, up_b, down_b = bufs[3 * half : 3 * half + 3]
        copies[3 * half].wait()
        gate = dot(x, gate_b[...], ((1,), (1,)))
        copies[3 * half + 1].wait()
        up = dot(x, up_b[...], ((1,), (1,)))
        hidden = (gate / (1.0 + jnp.exp(-gate)) * up).astype(BF16)
        copies[3 * half + 2].wait()
        part = dot(hidden, down_b[...])
        total = part if total is None else total + part
    total = total.astype(BF16)
    at = 0
    for o in outs:
        o[...] = total[at : at + o.shape[0]]
        at += o.shape[0]


def run_expert(xs, weights, parts=None):
    width = xs[0].shape[1]
    rows = sum(x.shape[0] for x in xs)
    parts = parts or [x.shape[0] for x in xs]
    any_spec = pl.BlockSpec(memory_space=pl.ANY)
    blocks = [pl.BlockSpec(x.shape, lambda: (0, 0)) for x in xs]
    return pl.pallas_call(
        functools.partial(expert_kernel, blocks=len(xs)),
        in_specs=blocks + [any_spec] * 6,
        out_specs=[pl.BlockSpec((n, width), lambda: (0, 0)) for n in parts],
        out_shape=[jax.ShapeDtypeStruct((n, width), BF16) for n in parts],
        scratch_shapes=[pltpu.VMEM(w.shape, BF16) for w in weights] + [pltpu.SemaphoreType.DMA((6,))],
        compiler_params=pltpu.CompilerParams(vmem_limit_bytes=VMEM_LIMIT),
        cost_estimate=pl.CostEstimate(
            flops=rows * sum(w.size for w in weights) * 2, transcendentals=0, bytes_accessed=sum(w.size for w in weights) * 2
        ),
        name="expert",
    )(*xs, *weights)


def ring(size, step):
    return [(i, (i + step) % size) for i in range(size)]


def add(*terms):
    return sum(t.astype(F32) for t in terms).astype(BF16)


def tie(*values):
    return lax.optimization_barrier(values)


def place_call(body, specs, out_block, out_shape):
    return pl.pallas_call(
        body,
        grid_spec=pltpu.PrefetchScalarGridSpec(num_scalar_prefetch=1, grid=(1,), in_specs=specs, out_specs=out_block),
        out_shape=out_shape,
        compiler_params=pltpu.CompilerParams(vmem_limit_bytes=VMEM_LIMIT),
    )


def shards(
    queries,
    keys,
    values,
    query_gain,
    key_gain,
    moe_input,
    expert_ids,
    route_weight,
    gate_weight,
    up_weight,
    down_weight,
    output_gain,
):
    seg_rows = queries.shape[0]
    half_rows = seg_rows // 2
    tok_rows, model_width = moe_input.shape
    experts = lax.axis_size("ep")
    column = lax.axis_index(TP)
    ep = lax.axis_index("ep")
    core = lax.axis_index("tp_1")
    key_head = column * KV // lax.axis_size(TP)
    place = jnp.stack([key_head // 2, key_head % 2, ep, core, column]).astype(jnp.int32)

    whole = lambda shape: pl.BlockSpec(shape, lambda i, p: (0, 0))
    own = whole((2, expert_ids.shape[0]))
    slots = experts * CAP
    outgoing = place_call(
        functools.partial(dispatch_kernel, experts=experts),
        [own, whole((tok_rows, model_width))],
        pl.BlockSpec((experts, CAP, model_width), lambda i, p: (0, 0, 0)),
        jax.ShapeDtypeStruct((experts, CAP, model_width), BF16),
    )(place, expert_ids.T, moe_input)
    arrived = lax.all_to_all(outgoing, "ep", split_axis=0, concat_axis=0, tiled=True).reshape(slots, model_width)
    swap = [(0, 1), (1, 0)]

    row_table = jnp.asarray(angle_tables(seg_rows * experts // GRID_W))
    col_table = jnp.asarray(angle_tables(GRID_W))
    kv_grid = half_rows // GRID_W
    kv_rows = pl.BlockSpec((half_rows, 128), lambda i, p: (p[3], p[0]))
    arrived, keys = tie(arrived, keys)
    kv_own = place_call(
        key_kernel,
        [
            kv_rows,
            kv_rows,
            whole((1, HD)),
            pl.BlockSpec((kv_grid, 2 * PAIRS), lambda i, p: (2 * p[2] + p[3], 0)),
            whole((GRID_W, 2 * PAIRS)),
        ],
        pl.BlockSpec((experts, half_rows, 2 * HD), lambda i, p: (0, 0, 0)),
        jax.ShapeDtypeStruct((experts, half_rows, 2 * HD), BF16),
    )(place, keys, values, key_gain[None], row_table, col_table)
    kv_near = lax.all_to_all(kv_own, "ep", split_axis=0, concat_axis=0, tiled=True)
    kv_near = kv_near.reshape(-1, 2 * HD)

    half = slots // 2

    def exchange(up, down):
        up = lax.ppermute(up, "tp_0", ring(8, 1))
        down = lax.ppermute(down, "tp_0", ring(8, -1))
        return up, down

    r1, l1 = exchange(arrived, arrived)
    r1, l1, gate_weight, up_weight, down_weight, queries = tie(r1, l1, gate_weight, up_weight, down_weight, queries)
    own_weights = (gate_weight[0].T, up_weight[0].T, down_weight[0])
    weights = own_weights + tuple(lax.ppermute(w, "tp_1", swap) for w in own_weights)
    r2, l2 = exchange(r1, l1)
    q = place_call(
        query_kernel,
        [
            whole((HD, seg_rows)),
            whole((1, HD)),
            pl.BlockSpec((seg_rows // GRID_W, 2 * PAIRS), lambda i, p: (p[2], 0)),
            whole((GRID_W, 2 * PAIRS)),
        ],
        whole((seg_rows, 2 * HD)),
        jax.ShapeDtypeStruct((seg_rows, 2 * HD), BF16),
    )(place, queries.T, query_gain[None], row_table, col_table)
    r3, l3 = exchange(r2, l2)
    p0, pr1, pl1, pr2, pl2 = run_expert((arrived, r1, l1, r2, l2), weights)
    r3, l3, p0 = tie(r3, l3, p0)
    r4, l4 = exchange(r3[:half], l3[half:])
    p0, kv_near = tie(p0, kv_near)
    kv_far = lax.ppermute(kv_near, "tp_1", swap)
    pr4, pl4, pr3, pl3 = run_expert((r4, l4, r3, l3), weights)
    pr4, pl4, kv_near = tie(pr4, pl4, kv_near)
    a1, b1 = exchange(pl4, pr4)
    state = attend(q, kv_near, 0, 4096)
    a1, b1, state = tie(a1, b1, state)
    a2 = add(pl3, jnp.pad(a1, ((half, 0), (0, 0))))
    b2 = add(pr3, jnp.pad(b1, ((0, half), (0, 0))))
    a2, b2, state = tie(a2, b2, state)
    a2, b2 = exchange(a2, b2)
    state = attend(q, kv_near, 4096, 4096, state)
    a2, b2, state = tie(a2, b2, state)
    a3, b3 = add(pl2, a2), add(pr2, b2)
    a3, b3, state = tie(a3, b3, state)
    a3, b3 = exchange(a3, b3)
    state = attend(q, kv_far, 0, 4096, state)
    a3, b3, state = tie(a3, b3, state)
    a4, b4 = add(pl1, a3), add(pr1, b3)
    a4, b4, state = tie(a4, b4, state)
    a4, b4 = exchange(a4, b4)
    attended = attend(q, kv_far, 4096, 4096, state, last=True)
    a4, b4, attended = tie(a4, b4, attended)
    attended = attended.T
    expert_out = add(p0, a4, b4)
    returned = lax.all_to_all(
        expert_out.reshape(experts, CAP, model_width), "ep", split_axis=0, concat_axis=0, tiled=True
    ).reshape(slots, model_width)
    moe_output = place_call(
        functools.partial(combine_kernel, experts=experts),
        [own, own, whole((tok_rows, model_width)), whole((slots, model_width)), whole((1, model_width))],
        whole((tok_rows, model_width)),
        jax.ShapeDtypeStruct((tok_rows, model_width), BF16),
    )(place, expert_ids.T, route_weight.T, moe_input, returned, output_gain[None])
    return (attended, moe_output)


def solution(mesh):
    split = Mesh(mesh.devices.reshape(mesh.shape["ep"], 8, 2), ("ep", "tp_0", "tp_1"))
    return jax.shard_map(
        shards,
        mesh=split,
        in_specs=(
            P("ep", TP),
            P("ep", None),
            P("ep", None),
            P(),
            P(),
            P(EP_TP, None),
            P("ep", None),
            P("ep", None),
            P("ep", None, TP),
            P("ep", None, TP),
            P("ep", TP, None),
            P(),
        ),
        out_specs=(P("ep", TP), P(EP_TP, None)),
        check_vma=False,
    )
```

```python
import functools
import math

import jax
import jax.numpy as jnp
import numpy as np
from jax import lax
from jax.experimental import pallas as pl
from jax.experimental.pallas import tpu as pltpu
from jax.sharding import Mesh
from jax.sharding import PartitionSpec as P


KV = 4
GRID_W = 64
TP = ("tp_0", "tp_1")
EP_TP = ("ep", "tp_0", "tp_1")
CAP = 7
HD = 64
HALF = HD // 2
PAIRS = HD // 4
LOG2E = math.log2(math.e)

rope_theta = 10000.0
rms_epsilon = 1e-06
norm_epsilon = 1e-05
residual_scale = 1.4142135623730951

F32 = jnp.float32
BF16 = jnp.bfloat16
VMEM_LIMIT = 56 * 1024 * 1024


def dot(a, b, contract=((1,), (0,))):
    return lax.dot_general(a, b, (contract, ((), ())), preferred_element_type=F32)


def angle_tables(count):
    inverse = (np.float32(rope_theta) ** (-np.arange(PAIRS, dtype=np.float32) / np.float32(PAIRS))).astype(np.float32)
    angles = np.arange(count, dtype=np.float32)[:, None] * inverse
    return np.concatenate([np.cos(angles), np.sin(angles)], axis=1).astype(np.float32)


def spread(row_table, col_table):
    rows = row_table.shape[0]
    width = row_table.shape[1]
    by_row = jnp.broadcast_to(row_table[:, None, :], (rows, GRID_W, width)).reshape(rows * GRID_W, width)
    by_col = jnp.broadcast_to(col_table[None, :, :], (rows, GRID_W, width)).reshape(rows * GRID_W, width)
    cosines = jnp.concatenate([by_row[:, :PAIRS], by_col[:, :PAIRS]], axis=1)
    sines = jnp.concatenate([by_row[:, PAIRS:], by_col[:, PAIRS:]], axis=1)
    return cosines, sines


def rotate(heads, gain, cosines, sines):
    squares = jnp.mean(heads * heads, axis=-1, keepdims=True)
    heads = heads * lax.rsqrt(squares + rms_epsilon) * gain
    a = heads[:, :HALF]
    b = heads[:, HALF:]
    return jnp.concatenate([a * cosines - b * sines, b * cosines + a * sines], axis=1)


def key_kernel(place, keys, values, gain, row_table, col_table, out):
    low = place[1] == 0
    k = jnp.where(low, keys[:, :HD], keys[:, HD:]).astype(F32)
    v = jnp.where(low, values[:, :HD], values[:, HD:])
    cosines, sines = spread(row_table[...], col_table[...])
    kv = jnp.concatenate([rotate(k, gain[...], cosines, sines).astype(BF16), v], axis=1)

    def copy(i, carry):
        out[i] = kv
        return carry

    lax.fori_loop(0, out.shape[0], copy, 0)


def query_kernel(place, queries, gain, row_table, col_table, out):
    cosines, sines = spread(row_table[...], col_table[...])
    q = rotate(queries[...].astype(F32).T, gain[...], cosines, sines).astype(BF16)
    scaled = q.astype(F32) * F32(LOG2E * HD**-0.5)
    high = scaled.astype(BF16)
    out[...] = jnp.concatenate([high, (scaled - high.astype(F32)).astype(BF16)], axis=1)


def attend_kernel(*refs, block_q, block_k, first, last):
    q_ref, kv_ref = refs[:2]
    state_ref, out_ref = (None, refs[2]) if first else refs[2:4]
    kk_ref, v1_ref, top_ref, acc_ref, part_ref = refs[-5:]
    keys = kk_ref.shape[0]
    count = keys // block_k
    rows_all = q_ref.shape[0]
    lane = lax.broadcasted_iota(jnp.int32, (512, 128), 1)

    def stage(i, carry):
        rows = pl.ds(pl.multiple_of(i * 512, 512), 512)
        kv = kv_ref[rows, :]
        kk_ref[rows, :] = jnp.concatenate([kv[:, :HD], kv[:, :HD]], axis=1)
        v1_ref[rows, :] = jnp.where(lane < HD, jnp.ones_like(kv), kv)
        return carry

    lax.fori_loop(0, keys // 512, stage, 0)

    def start(t, carry):
        rows = pl.ds(pl.multiple_of(t * 256, 256), 256)
        if first:
            s = dot(q_ref[rows, :], kk_ref[:256, :], ((1,), (1,)))
            top = jnp.max(s, axis=1, keepdims=True)
        else:
            acc = state_ref[rows, :]
            acc_ref[rows, :] = acc
            top = acc[:, 1:2]
        top_ref[rows, :] = jnp.broadcast_to(top, (256, 128))
        return carry

    lax.fori_loop(0, rows_all // 256, start, 0)
    if first:
        acc_ref[...] = jnp.zeros_like(acc_ref)
    part_ref[...] = jnp.zeros_like(part_ref)

    def weigh(q, top, at):
        s = dot(q, kk_ref[pl.ds(at, 256), :], ((1,), (1,)))
        p = jnp.exp2(s - jnp.concatenate([top, top], axis=1)).astype(BF16)
        return dot(p, v1_ref[pl.ds(at, 256), :])

    def tile(i, carry):
        rows = pl.ds(pl.multiple_of(i // count * block_q, block_q), block_q)
        at = i % count * block_k
        q = q_ref[rows, :]
        top = top_ref[rows, :]
        part = jnp.zeros((block_q, 128), F32)
        for k in range(block_k // 256):
            part = part + weigh(q, top, pl.multiple_of(at + k * 256, 256))
        part_ref[rows, :] += part
        return carry

    lax.fori_loop(0, rows_all // block_q * count, tile, 0)
    over = jnp.max(jnp.where(part_ref[:, :1] < 2.0**100, 0.0, 1.0)) > 0

    @pl.when(over)
    def _():
        def again(r, carry):
            rows = pl.ds(pl.multiple_of(r * 128, 128), 128)
            q = q_ref[rows, :]
            top = top_ref[rows, :]

            def raise_top(k, peak):
                s = dot(q, kk_ref[pl.ds(pl.multiple_of(k * 256, 256), 256), :], ((1,), (1,)))
                return jnp.maximum(peak, jnp.max(s, axis=1, keepdims=True))

            peak = lax.fori_loop(0, keys // 256, raise_top, jnp.max(top, axis=1, keepdims=True))
            peak = jnp.broadcast_to(peak, (128, 128))
            acc_ref[rows, :] = acc_ref[rows, :] * jnp.exp2(top - peak)
            top_ref[rows, :] = peak
            part_ref[rows, :] = jnp.zeros((128, 128), F32)

            def add(k, carry):
                part_ref[rows, :] += weigh(q, peak, pl.multiple_of(k * 256, 256))
                return carry

            return lax.fori_loop(0, keys // 256, add, carry)

        lax.fori_loop(0, rows_all // 128, again, 0)

    acc = acc_ref[...] + part_ref[...]
    if last:
        out_ref[...] = (acc[:, HD:] / acc[:, :1]).T.astype(BF16)
    else:
        at = lax.broadcasted_iota(jnp.int32, acc.shape, 1)
        out_ref[...] = jnp.where(at == 1, top_ref[...], acc)


def attend(q, kv, start, keys, state=None, last=False, block_q=512, block_k=2048):
    rows = q.shape[0]
    whole = pl.BlockSpec((rows, 128), lambda j: (0, 0))
    if last:
        out_shape = jax.ShapeDtypeStruct((HD, rows), BF16)
        out_specs = pl.BlockSpec((HD, rows), lambda j: (0, 0))
    else:
        out_shape = jax.ShapeDtypeStruct((rows, 128), F32)
        out_specs = whole
    return pl.pallas_call(
        functools.partial(attend_kernel, block_q=block_q, block_k=block_k, first=state is None, last=last),
        grid=(1,),
        in_specs=[whole, pl.BlockSpec((keys, 128), lambda j: (start // keys, 0))] + [whole] * (state is not None),
        out_specs=out_specs,
        out_shape=out_shape,
        scratch_shapes=[pltpu.VMEM((keys, 128), BF16)] * 2 + [pltpu.VMEM((rows, 128), F32)] * 3,
        compiler_params=pltpu.CompilerParams(vmem_limit_bytes=VMEM_LIMIT),
        cost_estimate=pl.CostEstimate(flops=rows * keys * 2 * 256 * 2, transcendentals=0, bytes_accessed=keys * 256),
        name="attend",
    )(q, kv, *(() if state is None else (state,)))


def own_tokens(place, table, tokens):
    width = table.shape[1]
    start = place[4] * tokens
    return pltpu.roll(table[...], jnp.where(start == 0, 0, width - start), 1)[:, :tokens]


def slots_of(ids, experts):
    tokens = ids.shape[1]
    width = experts * CAP
    slot = lax.broadcasted_iota(jnp.int32, (width, tokens), 0)
    owner = jnp.zeros((width, tokens), jnp.int32)
    for e in range(1, experts):
        owner = owner + (slot >= e * CAP).astype(jnp.int32)
    first = ids[0:1, :] == owner
    second = ids[1:2, :] == owner
    named = jnp.where(first | second, 1.0, 0.0)
    row = lax.broadcasted_iota(jnp.int32, (tokens, tokens), 0)
    col = lax.broadcasted_iota(jnp.int32, (tokens, tokens), 1)
    before = dot(named.astype(BF16), jnp.where(row < col, 1.0, 0.0).astype(BF16))
    rank = (slot - owner * CAP).astype(F32)
    taken = (named > 0) & (before == rank)
    return taken, first


def dispatch_kernel(place, ids, rows, out, *, experts):
    taken, _ = slots_of(own_tokens(place, ids, rows.shape[0]), experts)
    picked = dot(jnp.where(taken, 1.0, 0.0).astype(BF16), rows[...])
    for e in range(experts):
        out[e] = picked[e * CAP : (e + 1) * CAP].astype(BF16)


def combine_kernel(place, ids, weights, rows, returned, gain, out, *, experts):
    tokens = rows.shape[0]
    taken, first = slots_of(own_tokens(place, ids, tokens), experts)
    w = own_tokens(place, weights, tokens)
    scale = jnp.where(taken, jnp.where(first, w[0:1, :], w[1:2, :]), 0.0)
    high = scale.astype(BF16)
    rest = scale - high.astype(F32)
    mid = rest.astype(BF16)
    low = (rest - mid.astype(F32)).astype(BF16)
    back = returned[...]
    down = ((0,), (0,))
    mixed = residual_scale * rows[...].astype(F32) + (dot(high, back, down) + dot(mid, back, down) + dot(low, back, down))
    average = jnp.mean(mixed, axis=-1, keepdims=True)
    centered = mixed - average
    variance = jnp.mean(centered * centered, axis=-1, keepdims=True)
    out[...] = (centered * lax.rsqrt(variance + norm_epsilon) * gain[...]).astype(BF16)


def expert_kernel(*refs, blocks):
    xs, weights, outs = refs[:blocks], refs[blocks : blocks + 6], refs[blocks + 6 : -6]
    x_ref, gate_b, up_b, down_b, total_ref, sems = refs[-6:]
    chunks, width = gate_b.shape[:2]
    each = chunks // 2
    copies = []
    for c in range(chunks):
        rows = pl.ds(c % each * width, width)
        for i, buf in enumerate((gate_b, up_b, down_b)):
            source = weights[3 * (c // each) + i]
            copies.append(pltpu.make_async_copy(source.at[rows], buf.at[c], sems.at[i, c]))
    for copy in copies:
        copy.start()
    at = 0
    for x in xs:
        x_ref[pl.ds(at, x.shape[0]), :] = x[...]
        at += x.shape[0]

    def arrive(i, c, buf):
        pltpu.make_async_copy(buf.at[c], buf.at[c], sems.at[i, c]).wait()

    def chunk(c, carry):
        x = x_ref[...]
        arrive(0, c, gate_b)
        gate = dot(x, gate_b[c], ((1,), (1,)))
        arrive(1, c, up_b)
        up = dot(x, up_b[c], ((1,), (1,)))
        hidden = (gate / (1.0 + jnp.exp(-gate)) * up).astype(BF16)
        arrive(2, c, down_b)
        part = dot(hidden, down_b[c])

        @pl.when(c == 0)
        def _():
            total_ref[...] = part

        @pl.when(c == 1)
        def _():
            total = (total_ref[...] + part).astype(BF16)
            at = 0
            for o in outs:
                o[...] = total[at : at + o.shape[0]]
                at += o.shape[0]

        return carry

    lax.fori_loop(0, chunks, chunk, 0)


def run_expert(xs, weights, chunks=2):
    width = xs[0].shape[1]
    rows = sum(x.shape[0] for x in xs)
    hidden = weights[0].shape[0] * 2 // chunks
    blocks = [pl.BlockSpec(x.shape, lambda: (0, 0)) for x in xs]
    return pl.pallas_call(
        functools.partial(expert_kernel, blocks=len(xs)),
        in_specs=blocks + [pl.BlockSpec(memory_space=pl.ANY)] * 6,
        out_specs=blocks,
        out_shape=[jax.ShapeDtypeStruct(x.shape, BF16) for x in xs],
        scratch_shapes=[pltpu.VMEM((rows, width), BF16)]
        + [pltpu.VMEM((chunks, hidden, width), BF16)] * 3
        + [pltpu.VMEM((rows, width), F32), pltpu.SemaphoreType.DMA((3, chunks))],
        compiler_params=pltpu.CompilerParams(vmem_limit_bytes=VMEM_LIMIT),
        cost_estimate=pl.CostEstimate(
            flops=rows * sum(w.size for w in weights) * 2, transcendentals=0, bytes_accessed=sum(w.size for w in weights) * 2
        ),
        name="expert",
    )(*xs, *weights)


def ring(size, step):
    return [(i, (i + step) % size) for i in range(size)]


def add(*terms):
    return sum(t.astype(F32) for t in terms).astype(BF16)


def tie(*values):
    return lax.optimization_barrier(values)


def place_call(body, specs, out_block, out_shape):
    return pl.pallas_call(
        body,
        grid_spec=pltpu.PrefetchScalarGridSpec(num_scalar_prefetch=1, grid=(1,), in_specs=specs, out_specs=out_block),
        out_shape=out_shape,
        compiler_params=pltpu.CompilerParams(vmem_limit_bytes=VMEM_LIMIT),
    )


def shards(
    queries,
    keys,
    values,
    query_gain,
    key_gain,
    moe_input,
    expert_ids,
    route_weight,
    gate_weight,
    up_weight,
    down_weight,
    output_gain,
):
    seg_rows = queries.shape[0]
    half_rows = seg_rows // 2
    tok_rows, model_width = moe_input.shape
    experts = lax.axis_size("ep")
    column = lax.axis_index(TP)
    ep = lax.axis_index("ep")
    core = lax.axis_index("tp_1")
    key_head = column * KV // lax.axis_size(TP)
    place = jnp.stack([key_head // 2, key_head % 2, ep, core, column]).astype(jnp.int32)

    whole = lambda shape: pl.BlockSpec(shape, lambda i, p: (0, 0))
    own = whole((2, expert_ids.shape[0]))
    slots = experts * CAP
    outgoing = place_call(
        functools.partial(dispatch_kernel, experts=experts),
        [own, whole((tok_rows, model_width))],
        pl.BlockSpec((experts, CAP, model_width), lambda i, p: (0, 0, 0)),
        jax.ShapeDtypeStruct((experts, CAP, model_width), BF16),
    )(place, expert_ids.T, moe_input)
    arrived = lax.all_to_all(outgoing, "ep", split_axis=0, concat_axis=0, tiled=True).reshape(slots, model_width)
    swap = [(0, 1), (1, 0)]

    row_table = jnp.asarray(angle_tables(seg_rows * experts // GRID_W))
    col_table = jnp.asarray(angle_tables(GRID_W))
    kv_grid = half_rows // GRID_W
    kv_rows = pl.BlockSpec((half_rows, 128), lambda i, p: (p[3], p[0]))
    arrived, keys = tie(arrived, keys)
    kv_own = place_call(
        key_kernel,
        [
            kv_rows,
            kv_rows,
            whole((1, HD)),
            pl.BlockSpec((kv_grid, 2 * PAIRS), lambda i, p: (2 * p[2] + p[3], 0)),
            whole((GRID_W, 2 * PAIRS)),
        ],
        pl.BlockSpec((experts, half_rows, 2 * HD), lambda i, p: (0, 0, 0)),
        jax.ShapeDtypeStruct((experts, half_rows, 2 * HD), BF16),
    )(place, keys, values, key_gain[None], row_table, col_table)
    kv_near = lax.all_to_all(kv_own, "ep", split_axis=0, concat_axis=0, tiled=True)
    kv_near = kv_near.reshape(-1, 2 * HD)

    half = slots // 2

    def exchange(up, down):
        up = lax.ppermute(up, "tp_0", ring(8, 1))
        down = lax.ppermute(down, "tp_0", ring(8, -1))
        return up, down

    r1, l1 = exchange(arrived, arrived)
    r1, l1, gate_weight, up_weight, down_weight, queries = tie(r1, l1, gate_weight, up_weight, down_weight, queries)
    own_weights = (gate_weight[0].T, up_weight[0].T, down_weight[0])
    weights = own_weights + tuple(lax.ppermute(w, "tp_1", swap) for w in own_weights)
    r2, l2 = exchange(r1, l1)
    q = place_call(
        query_kernel,
        [
            whole((HD, seg_rows)),
            whole((1, HD)),
            pl.BlockSpec((seg_rows // GRID_W, 2 * PAIRS), lambda i, p: (p[2], 0)),
            whole((GRID_W, 2 * PAIRS)),
        ],
        whole((seg_rows, 2 * HD)),
        jax.ShapeDtypeStruct((seg_rows, 2 * HD), BF16),
    )(place, queries.T, query_gain[None], row_table, col_table)
    r3, l3 = exchange(r2, l2)
    p0, pr1, pl1 = run_expert((arrived, r1, l1), weights)
    r3, l3, p0 = tie(r3, l3, p0)
    r4, l4 = exchange(r3[:half], l3[half:])
    p0, kv_near = tie(p0, kv_near)
    kv_far = lax.ppermute(kv_near, "tp_1", swap)
    pr4, pl4, pr3, pl3, pr2, pl2 = run_expert((r4, l4, r3, l3, r2, l2), weights)
    pr4, pl4, kv_near = tie(pr4, pl4, kv_near)
    a1, b1 = exchange(pl4, pr4)
    state = attend(q, kv_near, 0, 4096)
    a1, b1, state = tie(a1, b1, state)
    a2 = add(pl3, jnp.pad(a1, ((half, 0), (0, 0))))
    b2 = add(pr3, jnp.pad(b1, ((0, half), (0, 0))))
    a2, b2, state = tie(a2, b2, state)
    a2, b2 = exchange(a2, b2)
    state = attend(q, kv_near, 4096, 4096, state)
    a2, b2, state = tie(a2, b2, state)
    a3, b3 = add(pl2, a2), add(pr2, b2)
    a3, b3, state = tie(a3, b3, state)
    a3, b3 = exchange(a3, b3)
    state = attend(q, kv_far, 0, 4096, state)
    a3, b3, state = tie(a3, b3, state)
    a4, b4 = add(pl1, a3), add(pr1, b3)
    a4, b4, state = tie(a4, b4, state)
    a4, b4 = exchange(a4, b4)
    attended = attend(q, kv_far, 4096, 4096, state, last=True)
    a4, b4, attended = tie(a4, b4, attended)
    attended = attended.T
    expert_out = add(p0, a4, b4)
    returned = lax.all_to_all(
        expert_out.reshape(experts, CAP, model_width), "ep", split_axis=0, concat_axis=0, tiled=True
    ).reshape(slots, model_width)
    moe_output = place_call(
        functools.partial(combine_kernel, experts=experts),
        [own, own, whole((tok_rows, model_width)), whole((slots, model_width)), whole((1, model_width))],
        whole((tok_rows, model_width)),
        jax.ShapeDtypeStruct((tok_rows, model_width), BF16),
    )(place, expert_ids.T, route_weight.T, moe_input, returned, output_gain[None])
    return (attended, moe_output)


def solution(mesh):
    split = Mesh(mesh.devices.reshape(mesh.shape["ep"], 8, 2), ("ep", "tp_0", "tp_1"))
    return jax.shard_map(
        shards,
        mesh=split,
        in_specs=(
            P("ep", TP),
            P("ep", None),
            P("ep", None),
            P(),
            P(),
            P(EP_TP, None),
            P("ep", None),
            P("ep", None),
            P("ep", None, TP),
            P("ep", None, TP),
            P("ep", TP, None),
            P(),
        ),
        out_specs=(P("ep", TP), P(EP_TP, None)),
        check_vma=False,
    )
```
